32 devices in a mesh: sp: 16 (over z, y, x), tp: 2 (over core).
Axes of the slice: x: 2, y: 2, z: 4, core: 2. Of those that a mesh axis runs over, the one named last changes fastest.
Arguments:
- stream: bfloat16 [6144, 2048], P('sp', 'tp'), may hold values from -6 to 6
- norm_gain: float32 [2, 2048], replicated, may hold values from 0.1 to 1.9
- a_weight: bfloat16 [2, 2048, 2048], P(None, 'sp', 'tp'), may hold values from -0.125 to 0.125
- gate_weight: bfloat16 [2, 2048, 2048], P(None, 'sp', 'tp'), may hold values from -0.125 to 0.125
- conv_weight: float32 [2, 31, 2048], P(None, None, 'tp'), may hold values from -4 to 4, as said below
- conv_bias: float32 [2, 2048], P(None, 'tp'), may hold values from -3 to 3
- ln_gain: float32 [2, 2048], P(None, 'tp'), may hold values from 0.1 to 1.9
- ln_shift: float32 [2, 2048], P(None, 'tp'), may hold values from -3 to 3
- out_weight: bfloat16 [2, 2048, 2048], P(None, 'sp', 'tp'), may hold values from -0.125 to 0.125
Outputs:
- result: bfloat16 [6144, 2048], P('sp', 'tp')
The draws below stay inside these ranges and needn't reach their ends.
Inputs may be any that keep to these rules, and one draw needn't show every extreme that they name: `conv_weight`: each column is drawn with its own scale, and blocks of 16 channels differ in scale by up to a factor of nine.
All inputs are finite; a program needn't handle non-finite values.
Results may differ from the reference program's by a relative error of at most 0.01.
Values may be sent and summed in bfloat16 or wider, within the bound.
A program may use at most 64 MiB of HBM per device.

```python
import jax
import jax.numpy as jnp
from jax import lax

D = 2048
WIDTH = 31
LAYERS = 2
TOKENS = 6144


def draw_conv_weight(key, part):
    first = jax.random.fold_in(key, 11)
    second = jax.random.fold_in(key, 12)
    values = jnp.clip(jax.random.normal(first, (LAYERS, WIDTH, D), jnp.float32), -6.0, 6.0)
    block_scale = jnp.exp(jax.random.uniform(second, (LAYERS, 1, D // 16), jnp.float32, -1.09, 1.09))
    spread_scale = jnp.repeat(block_scale, 16, axis=2)
    return values * spread_scale * WIDTH ** (-0.5)


def shard_levels(key, shape, cuts, smallest, high):
    level = 1.0
    for dim, blocks in cuts:
        steps = jax.random.uniform(jax.random.fold_in(jax.random.fold_in(key, 6), dim), (blocks,), jnp.float32, smallest / len(cuts), high / len(cuts))
        level = level * jnp.repeat(jnp.exp(steps), shape[dim] // blocks).reshape((-1,) + (1,) * (len(shape) - 1 - dim))
    return level


def normal_values(stream_key, dims, spread, most, shards=(), kind=jnp.bfloat16):
    drawn = jax.random.normal(stream_key, dims, jnp.float32) * spread
    if len(shards) > 0:
        drawn = shard_levels(stream_key, dims, shards, -0.22, 0.18) * drawn
    return jnp.clip(drawn, min=-most, max=most).astype(kind)


def setup_inputs(seed: int = 0) -> dict:
    arg_keys = jax.random.split(jax.random.key(seed), 10)
    return {
        "stream": normal_values(arg_keys[0], (TOKENS, D), 1.0, 6.0, ((0, 16), (1, 2))),
        "norm_gain": jnp.clip(1.0 + 0.18 * jax.random.normal(arg_keys[1], (LAYERS, D), jnp.float32), 0.1, 1.9),
        "a_weight": normal_values(arg_keys[2], (LAYERS, D, D), D ** -0.5, 0.125, ((1, 16), (2, 2))),
        "gate_weight": normal_values(arg_keys[3], (LAYERS, D, D), D ** -0.5, 0.125, ((1, 16), (2, 2))),
        "conv_weight": draw_conv_weight(jax.random.fold_in(arg_keys[9], 71), 0),
        "conv_bias": normal_values(arg_keys[5], (LAYERS, D), 0.5, 3.0, ((1, 2),), jnp.float32),
        "ln_gain": jnp.clip(1.0 + 0.18 * jax.random.normal(arg_keys[6], (LAYERS, D), jnp.float32), 0.1, 1.9),
        "ln_shift": normal_values(arg_keys[7], (LAYERS, D), 0.5, 3.0, ((1, 2),), jnp.float32),
        "out_weight": normal_values(arg_keys[8], (LAYERS, D, D), D ** -0.5, 0.125, ((1, 16), (2, 2))),
    }


EPSILON = 1e-06

def normalize_rows(stream_f, gain):
    factor = lax.rsqrt(lax.optimization_barrier(jnp.mean(stream_f * stream_f, axis=1, keepdims=True)) + EPSILON)
    return (stream_f * factor * gain[None, :]).astype(jnp.bfloat16)

def convolve(padded, kernel, conv_shift, out_rows):
    summed = jnp.zeros((out_rows, padded.shape[1]), jnp.float32) + conv_shift[None, :]
    for offset in range(kernel.shape[0]):
        window = lax.slice_in_dim(padded, offset, offset + out_rows, axis=0).astype(jnp.float32)
        summed = summed + window * kernel[offset][None, :]
    return summed

def finish_norm(conv_out, row_sum, row_squares, gain, shift):
    average = row_sum / D
    variance = row_squares / D - average * average
    normed = (conv_out - average) * lax.rsqrt(variance + EPSILON) * gain[None, :] + shift[None, :]
    return jax.nn.silu(normed).astype(jnp.bfloat16)

def reference(stream, norm_gain, a_weight, gate_weight, conv_weight, conv_bias, ln_gain, ln_shift, out_weight):
    reach = (WIDTH - 1) // 2
    current = stream
    for layer_index in range(LAYERS):
        stream_f = current.astype(jnp.float32)
        normed = normalize_rows(stream_f, norm_gain[layer_index])
        linear = jnp.dot(normed, a_weight[layer_index], preferred_element_type=jnp.float32)
        gating = jnp.dot(normed, gate_weight[layer_index], preferred_element_type=jnp.float32)
        gated = (linear * jax.nn.sigmoid(gating)).astype(jnp.bfloat16)
        padded = jnp.pad(gated, ((reach, reach), (0, 0)))
        conv_out = convolve(padded, conv_weight[layer_index], conv_bias[layer_index], TOKENS)
        row_sum = lax.optimization_barrier(jnp.sum(conv_out, axis=1, keepdims=True))
        row_squares = lax.optimization_barrier(jnp.sum(conv_out * conv_out, axis=1, keepdims=True))
        mixed_in = finish_norm(conv_out, row_sum, row_squares, ln_gain[layer_index], ln_shift[layer_index])
        branch = jnp.dot(mixed_in, out_weight[layer_index], preferred_element_type=jnp.float32)
        current = (stream_f + branch).astype(jnp.bfloat16)
    return current
```

```python
import functools

import jax
import jax.numpy as jnp
from jax import lax
from jax.experimental import pallas as pl
from jax.experimental.pallas import tpu as pltpu
from jax.sharding import PartitionSpec as P

D = 2048


EPSILON = 1e-06
MESH = pl.DeviceIdType.MESH
LOOKAHEAD = 3
ORDERS = ((0, 1, 2), (0, 2, 1), (0, 1, 2), (0, 2, 1), (2, 0, 1), (1, 0, 2))


def grid_of(mesh):
    count = mesh.shape["sp"]
    row = mesh.devices[:, 0]
    coords = [getattr(device, "coords", None) for device in row]
    if any(c is None for c in coords):
        return (count // 4, 2, 2) if count % 4 == 0 else (count, 1, 1)
    sizes = tuple(len({c[axis] for c in coords}) for axis in (2, 1, 0))
    if sizes[0] * sizes[1] * sizes[2] != count:
        return (count, 1, 1)
    return sizes


def gather_kernel(sizes, halves, pieces, *refs):
    count = (len(refs) - 3) // 2
    ins, outs = refs[:count], refs[count : 2 * count]
    local_sem, send_sem, recv_sem = refs[2 * count :]
    me = lax.axis_index("sp")
    strides = (sizes[1] * sizes[2], sizes[2], 1)
    where = [lax.rem(me // strides[k], sizes[k]) for k in range(3)]
    half_rows = ins[0].shape[1] // halves

    def peer(axis, step):
        other = lax.rem(where[axis] + step, sizes[axis])
        return me + (other - where[axis]) * strides[axis]

    peers = [(axis, step) for axis in range(3) for step in range(1, sizes[axis])]
    barrier = pltpu.get_barrier_semaphore()
    for axis, step in peers:
        pl.semaphore_signal(barrier, inc=1, device_id={"sp": peer(axis, step)}, device_id_type=MESH)
    pl.semaphore_wait(barrier, len(peers))

    def rows_of(piece):
        return pl.ds(pieces[piece][2] * half_rows, half_rows)

    def block(piece, done):
        matrix, layer, _ = pieces[piece]
        index = [slice(None) if axis in done else where[axis] for axis in range(3)]
        return outs[matrix].at[(layer, *index, rows_of(piece), slice(None))]

    def local(piece):
        matrix, layer, _ = pieces[piece]
        return pltpu.make_async_copy(
            ins[matrix].at[layer, rows_of(piece), :], block(piece, ()), local_sem.at[piece]
        )

    def copies(piece, phase):
        matrix, layer, _ = pieces[piece]
        order = ORDERS[piece % len(ORDERS)]
        axis = order[phase]
        target = block(piece, order[:phase])
        source = ins[matrix].at[layer, rows_of(piece), :] if phase == 0 else target
        found = []
        for step in range(1, sizes[axis]):
            slot = peers.index((axis, step))
            found.append(
                pltpu.make_async_remote_copy(
                    src_ref=source,
                    dst_ref=target,
                    send_sem=send_sem.at[piece, slot],
                    recv_sem=recv_sem.at[piece, slot],
                    device_id={"sp": peer(axis, step)},
                    device_id_type=MESH,
                )
            )
        return found

    def start(piece, phase):
        if phase == 0:
            local(piece).start()
        for copy in copies(piece, phase):
            copy.start()

    def landed(piece, phase):
        if phase == 0:
            local(piece).wait()
        for copy in copies(piece, phase):
            copy.wait_recv()

    total = len(pieces)
    for piece in range(min(LOOKAHEAD, total)):
        start(piece, 0)
    for step in range(total + 1):
        if step + LOOKAHEAD < total:
            start(step + LOOKAHEAD, 0)
        if step < total:
            landed(step, 0)
            start(step, 1)
        if step >= 1:
            landed(step - 1, 1)
            start(step - 1, 2)
    for piece in range(total):
        landed(piece, 2)
        for phase in range(3):
            for copy in copies(piece, phase):
                copy.wait_send()


def gather_weights(sizes, weights, pieces, halves):
    layers, depth, columns = weights[0].shape
    slots = sum(size - 1 for size in sizes)
    full = (layers, *sizes, depth, columns)
    moved = sum(size - 1 for size in sizes)
    gathered = pl.pallas_call(
        functools.partial(gather_kernel, sizes, halves, pieces),
        out_shape=[jax.ShapeDtypeStruct(full, jnp.bfloat16)] * len(weights),
        in_specs=[pl.BlockSpec(memory_space=pltpu.VMEM)] * len(weights),
        out_specs=[pl.BlockSpec(memory_space=pl.ANY)] * len(weights),
        scratch_shapes=[
            pltpu.SemaphoreType.DMA((len(pieces),)),
            pltpu.SemaphoreType.DMA((len(pieces), slots)),
            pltpu.SemaphoreType.DMA((len(pieces), slots)),
        ],
        compiler_params=pltpu.CompilerParams(collective_id=0, has_side_effects=True),
    )(*weights)
    count = sizes[0] * sizes[1] * sizes[2]
    return [whole.reshape(layers, count * depth, columns) for whole in gathered]


def with_halo(block, sides, width):
    for axis, dim in sides:
        count = lax.axis_size(axis)
        forward = [(i, i + 1) for i in range(count - 1)]
        backward = [(target, source) for source, target in forward]
        low = lax.ppermute(
            lax.slice_in_dim(block, block.shape[dim] - width, None, axis=dim), axis, forward
        )
        high = lax.ppermute(lax.slice_in_dim(block, 0, width, axis=dim), axis, backward)
        block = jnp.concatenate([low, block, high], axis=dim)
    return block


def all_channels(block):
    if lax.axis_size("tp") != 2:
        return lax.all_gather(block, "tp", axis=1, tiled=True)
    other = lax.ppermute(block, "tp", [(0, 1), (1, 0)])
    first = lax.axis_index("tp") == 0
    return jnp.concatenate(
        [jnp.where(first, block, other), jnp.where(first, other, block)], axis=1
    )


def normalize_rows(stream_f, gain):
    factor = lax.rsqrt(jnp.mean(stream_f * stream_f, axis=1, keepdims=True) + EPSILON)
    return (stream_f * factor * gain[None, :]).astype(jnp.bfloat16)


def convolve(padded, kernel, conv_shift, out_rows):
    summed = jnp.zeros((out_rows, padded.shape[1]), jnp.float32) + conv_shift[None, :]
    for offset in range(kernel.shape[0]):
        window = lax.slice_in_dim(padded, offset, offset + out_rows, axis=0).astype(jnp.float32)
        summed = summed + window * kernel[offset][None, :]
    return summed


def finish_norm(conv_out, row_sum, row_squares, gain, shift):
    average = row_sum / D
    variance = row_squares / D - average * average
    normed = (conv_out - average) * lax.rsqrt(variance + EPSILON) * gain[None, :] + shift[None, :]
    return jax.nn.silu(normed).astype(jnp.bfloat16)


def local(
    sizes,
    stream,
    norm_gain,
    a_weight,
    gate_weight,
    conv_weight,
    conv_bias,
    ln_gain,
    ln_shift,
    out_weight,
):
    reach = (conv_weight.shape[1] - 1) // 2
    layer_total = a_weight.shape[0]
    halves = 2
    pieces = [
        (matrix, layer, half)
        for layer in range(layer_total)
        for matrix in range(3)
        for half in range(halves)
    ]
    gathered = gather_weights(sizes, (a_weight, gate_weight, out_weight), pieces, halves)
    current = stream
    for layer_index in range(layer_total):
        stream_f = current.astype(jnp.float32)
        full_rows = all_channels(current)
        normed = normalize_rows(full_rows.astype(jnp.float32), norm_gain[layer_index])
        linear = jnp.dot(normed, gathered[0][layer_index], preferred_element_type=jnp.float32)
        gating = jnp.dot(normed, gathered[1][layer_index], preferred_element_type=jnp.float32)
        product = linear * jax.nn.sigmoid(gating)
        gated = product.astype(jnp.bfloat16)
        padded = with_halo(gated, (("sp", 0),), reach)
        out_rows = padded.shape[0] - 2 * reach
        conv_out = convolve(padded, conv_weight[layer_index], conv_bias[layer_index], out_rows)
        row_sum, row_squares = lax.psum(
            (
                jnp.sum(conv_out, axis=1, keepdims=True),
                jnp.sum(conv_out * conv_out, axis=1, keepdims=True),
            ),
            "tp",
        )
        mixed_in = finish_norm(
            conv_out, row_sum, row_squares, ln_gain[layer_index], ln_shift[layer_index]
        )
        mixed_rows = all_channels(mixed_in)
        branch = jnp.dot(mixed_rows, gathered[2][layer_index], preferred_element_type=jnp.float32)
        current = (stream_f + branch).astype(jnp.bfloat16)
    return current


def solution(mesh):
    placed = (
        P("sp", "tp"),
        P(),
        P(None, "sp", "tp"),
        P(None, "sp", "tp"),
        P(None, None, "tp"),
        P(None, "tp"),
        P(None, "tp"),
        P(None, "tp"),
        P(None, "sp", "tp"),
    )
    return jax.shard_map(
        functools.partial(local, grid_of(mesh)),
        mesh=mesh,
        in_specs=placed,
        out_specs=P("sp", "tp"),
        check_vma=False,
    )
```

```python
import functools

import jax
import jax.numpy as jnp
from jax import lax
from jax.experimental import pallas as pl
from jax.experimental.pallas import tpu as pltpu
from jax.sharding import PartitionSpec as P

D = 2048


EPSILON = 1e-06
MESH = pl.DeviceIdType.MESH
LOOKAHEAD = 3
ROUND = 16
HALVES = 2
ORDERS = ((0, 1, 2), (0, 2, 1))


def grid_of(mesh):
    count = mesh.shape["sp"]
    row = mesh.devices[:, 0]
    coords = [getattr(device, "coords", None) for device in row]
    if any(c is None for c in coords):
        return (count // 4, 2, 2) if count % 4 == 0 else (count, 1, 1)
    sizes = tuple(len({c[axis] for c in coords}) for axis in (2, 1, 0))
    if sizes[0] * sizes[1] * sizes[2] != count:
        return (count, 1, 1)
    return sizes


def gather_kernel(sizes, pieces, count, *refs):
    ins, outs = refs[:count], refs[count:-3]
    local_sem, send_sem, recv_sem = refs[-3:]
    me = lax.axis_index("sp")
    strides = (sizes[1] * sizes[2], sizes[2], 1)
    where = [lax.rem(me // strides[k], sizes[k]) for k in range(3)]
    wide = ins[0].shape[2] // HALVES

    def peer(axis, step):
        other = lax.rem(where[axis] + step, sizes[axis])
        return me + (other - where[axis]) * strides[axis]

    peers = [(axis, step) for axis in range(3) for step in range(1, sizes[axis])]
    barrier = pltpu.get_barrier_semaphore()
    for axis, step in peers:
        pl.semaphore_signal(barrier, inc=1, device_id={"sp": peer(axis, step)}, device_id_type=MESH)
    pl.semaphore_wait(barrier, len(peers))

    def source(piece):
        matrix, layer, half = pieces[piece][:3]
        return ins[matrix].at[layer, :, pl.ds(half * wide, wide)]

    def block(piece, done):
        half, phases, out, slot = pieces[piece][2:]
        order = ORDERS[half]
        if phases == 3:
            index = [slice(None) if axis in done else where[axis] for axis in range(3)]
            return outs[out].at[(*index, slice(None), pl.ds(half * wide, wide))]
        index = [slice(None) if axis in done else where[axis] for axis in order[:2]]
        return outs[out].at[(slot, *index, slice(None), slice(None))]

    def local(piece):
        return pltpu.make_async_copy(source(piece), block(piece, ()), local_sem.at[piece])

    def copies(piece, phase):
        order = ORDERS[pieces[piece][2]]
        if phase >= pieces[piece][3]:
            return []
        axis = order[phase]
        target = block(piece, order[:phase])
        found = []
        for step in range(1, sizes[axis]):
            slot = peers.index((axis, step))
            found.append(
                pltpu.make_async_remote_copy(
                    src_ref=source(piece) if phase == 0 else target,
                    dst_ref=target,
                    send_sem=send_sem.at[piece, slot],
                    recv_sem=recv_sem.at[piece, slot],
                    device_id={"sp": peer(axis, step)},
                    device_id_type=MESH,
                )
            )
        return found

    def start(piece, phase):
        if phase == 0:
            local(piece).start()
        for copy in copies(piece, phase):
            copy.start()

    def landed(piece, phase):
        if phase == 0:
            local(piece).wait()
        for copy in copies(piece, phase):
            copy.wait_recv()

    total = len(pieces)
    for piece in range(min(LOOKAHEAD, total)):
        start(piece, 0)
    for step in range(total + 1):
        if step + LOOKAHEAD < total:
            start(step + LOOKAHEAD, 0)
        if step < total:
            landed(step, 0)
            start(step, 1)
        if step >= 1:
            landed(step - 1, 1)
            start(step - 1, 2)
    for piece in range(total):
        landed(piece, 2)
        for phase in range(3):
            for copy in copies(piece, phase):
                copy.wait_send()


def gather_weights(sizes, weights, deferred):
    layers, depth, columns = weights[0].shape
    whole = layers - 1 if deferred else layers
    shapes, pieces = [], []
    for layer in range(whole):
        for matrix in range(3):
            for half in range(HALVES):
                pieces.append((matrix, layer, half, 3, len(shapes), 0))
            shapes.append((*sizes, depth, columns))
    if deferred:
        base = len(shapes)
        for group, members in enumerate(((0, 1), (2,))):
            for half in range(HALVES):
                ahead = tuple(sizes[axis] for axis in ORDERS[half][:2])
                shapes.append((len(members), *ahead, depth, columns // HALVES))
            for slot, matrix in enumerate(members):
                for half in range(HALVES):
                    out = base + group * HALVES + half
                    pieces.append((matrix, whole, half, 2, out, slot))
    slots = sum(size - 1 for size in sizes)
    gathered = pl.pallas_call(
        functools.partial(gather_kernel, sizes, pieces, len(weights)),
        out_shape=[jax.ShapeDtypeStruct(shape, jnp.bfloat16) for shape in shapes],
        in_specs=[pl.BlockSpec(memory_space=pltpu.VMEM)] * len(weights),
        out_specs=[pl.BlockSpec(memory_space=pl.ANY)] * len(shapes),
        scratch_shapes=[
            pltpu.SemaphoreType.DMA((len(pieces),)),
            pltpu.SemaphoreType.DMA((len(pieces), slots)),
            pltpu.SemaphoreType.DMA((len(pieces), slots)),
        ],
        compiler_params=pltpu.CompilerParams(collective_id=0, has_side_effects=True),
    )(*weights)
    rows = sizes[0] * sizes[1] * sizes[2] * depth
    full = [gathered[k].reshape(rows, columns) for k in range(3 * whole)]
    return full, gathered[3 * whole :]


def last_hop(stage, sizes, half):
    axis = ORDERS[half][2]
    stride = (sizes[1] * sizes[2], sizes[2], 1)[axis]
    count = sizes[0] * sizes[1] * sizes[2]
    pairs = [(i, i + stride if (i // stride) % 2 == 0 else i - stride) for i in range(count)]
    return lax.ppermute(stage, "sp", pairs)


def split_channels(block, sizes, half):
    axis = ORDERS[half][2]
    count = sizes[0] * sizes[1] * sizes[2]
    depth = block.shape[1] // count
    stride = (sizes[1] * sizes[2], sizes[2], 1)[axis]
    sides = [
        jnp.concatenate(
            [block[:, i * depth : (i + 1) * depth] for i in range(count) if (i // stride) % 2 == side],
            axis=1,
        )
        for side in range(2)
    ]
    first = lax.rem(lax.axis_index("sp") // stride, 2) == 0
    return jnp.where(first, sides[0], sides[1]), jnp.where(first, sides[1], sides[0])


def split_dot(parts, own, other):
    return jnp.dot(
        parts[0], own.reshape(-1, own.shape[-1]), preferred_element_type=jnp.float32
    ) + jnp.dot(parts[1], other.reshape(-1, other.shape[-1]), preferred_element_type=jnp.float32)


def with_halo(block, width):
    count = lax.axis_size("sp")
    forward = [(i, i + 1) for i in range(count - 1)]
    backward = [(target, source) for source, target in forward]
    low = lax.ppermute(block[block.shape[0] - width :], "sp", forward)
    high = lax.ppermute(block[:width], "sp", backward)
    return jnp.concatenate([low, block, high], axis=0)


def all_channels(block):
    if lax.axis_size("tp") != 2:
        return lax.all_gather(block, "tp", axis=1, tiled=True)
    other = lax.ppermute(block, "tp", [(0, 1), (1, 0)])
    first = lax.axis_index("tp") == 0
    return jnp.concatenate(
        [jnp.where(first, block, other), jnp.where(first, other, block)], axis=1
    )


def normalize_rows(stream_f, gain):
    factor = lax.rsqrt(jnp.mean(stream_f * stream_f, axis=1, keepdims=True) + EPSILON)
    return (stream_f * factor * gain[None, :]).astype(jnp.bfloat16)


def convolve(padded, kernel, conv_shift, out_rows):
    summed = jnp.zeros((out_rows, padded.shape[1]), jnp.float32) + conv_shift[None, :]
    for offset in range(kernel.shape[0]):
        window = lax.slice_in_dim(padded, offset, offset + out_rows, axis=0).astype(jnp.float32)
        summed = summed + window * kernel[offset][None, :]
    return summed


def finish_norm(conv_out, row_sum, row_squares, gain, shift):
    average = row_sum / D
    variance = row_squares / D - average * average
    normed = (conv_out - average) * lax.rsqrt(variance + EPSILON) * gain[None, :] + shift[None, :]
    return jax.nn.silu(normed).astype(jnp.bfloat16)


def local(
    sizes,
    stream,
    norm_gain,
    a_weight,
    gate_weight,
    conv_weight,
    conv_bias,
    ln_gain,
    ln_shift,
    out_weight,
):
    reach = (conv_weight.shape[1] - 1) // 2
    margin = (reach + ROUND - 1) // ROUND * ROUND
    layer_total = a_weight.shape[0]
    rows = stream.shape[0]
    deferred = sizes[1] == 2 and sizes[2] == 2 and layer_total > 1
    full, stages = gather_weights(sizes, (a_weight, gate_weight, out_weight), deferred)
    hops = []
    token = lax.axis_index("sp") * rows
    everything = rows * lax.axis_size("sp")
    spread = with_halo(all_channels(stream), margin * layer_total)
    wide = stream.shape[1]
    current = lax.dynamic_slice_in_dim(spread, lax.axis_index("tp") * wide, wide, axis=1)
    for layer_index in range(layer_total):
        beyond = margin * (layer_total - layer_index)
        if layer_index > 0:
            index = token - beyond + lax.broadcasted_iota(jnp.int32, (current.shape[0], 1), 0)
            inside = (index >= 0) & (index < everything)
            current = jnp.where(inside, current, jnp.zeros_like(current))
            spread = all_channels(current)
        stream_f = current.astype(jnp.float32)
        normed = normalize_rows(spread.astype(jnp.float32), norm_gain[layer_index])
        late = deferred and layer_index == layer_total - 1
        if late:
            gated = []
            for half in range(HALVES):
                parts = split_channels(normed, sizes, half)
                own, other = stages[half], hops[half]
                linear = split_dot(parts, own[0], other[0])
                gating = split_dot(parts, own[1], other[1])
                gated.append((linear * jax.nn.sigmoid(gating)).astype(jnp.bfloat16))
            gated = jnp.concatenate(gated, axis=1)
        else:
            matrices = full[3 * layer_index : 3 * layer_index + 3]
            linear = jnp.dot(normed, matrices[0], preferred_element_type=jnp.float32)
            gating = jnp.dot(normed, matrices[1], preferred_element_type=jnp.float32)
            gated = (linear * jax.nn.sigmoid(gating)).astype(jnp.bfloat16)
        if deferred and layer_index == layer_total - 2:
            hops = [last_hop(stages[half], sizes, half) for half in range(HALVES)]
            held, gated = lax.optimization_barrier((stages[HALVES:], gated))
            hops += [last_hop(held[half], sizes, half) for half in range(HALVES)]
        out_rows = rows + 2 * (beyond - margin)
        conv_out = convolve(
            gated[margin - reach :], conv_weight[layer_index], conv_bias[layer_index], out_rows
        )
        row_sum, row_squares = lax.psum(
            (
                jnp.sum(conv_out, axis=1, keepdims=True),
                jnp.sum(conv_out * conv_out, axis=1, keepdims=True),
            ),
            "tp",
        )
        mixed_in = finish_norm(
            conv_out, row_sum, row_squares, ln_gain[layer_index], ln_shift[layer_index]
        )
        mixed_rows = all_channels(mixed_in)
        if late:
            branch = jnp.concatenate(
                [
                    split_dot(
                        split_channels(mixed_rows, sizes, half),
                        stages[HALVES + half][0],
                        hops[HALVES + half][0],
                    )
                    for half in range(HALVES)
                ],
                axis=1,
            )
        else:
            branch = jnp.dot(mixed_rows, matrices[2], preferred_element_type=jnp.float32)
        kept = lax.slice_in_dim(stream_f, margin, margin + out_rows, axis=0)
        current = (kept + branch).astype(jnp.bfloat16)
    return current


def solution(mesh):
    placed = (
        P("sp", "tp"),
        P(),
        P(None, "sp", "tp"),
        P(None, "sp", "tp"),
        P(None, None, "tp"),
        P(None, "tp"),
        P(None, "tp"),
        P(None, "tp"),
        P(None, "sp", "tp"),
    )
    return jax.shard_map(
        functools.partial(local, grid_of(mesh)),
        mesh=mesh,
        in_specs=placed,
        out_specs=P("sp", "tp"),
        check_vma=False,
    )
```

```python
import functools

import jax
import jax.numpy as jnp
from jax import lax
from jax.experimental import pallas as pl
from jax.experimental.pallas import tpu as pltpu
from jax.sharding import PartitionSpec as P

D = 2048


EPSILON = 1e-06
MESH = pl.DeviceIdType.MESH
LOOKAHEAD = 3
ROUND = 16
HALVES = 2
ORDERS = ((0, 1, 2), (0, 2, 1))


def grid_of(mesh):
    count = mesh.shape["sp"]
    row = mesh.devices[:, 0]
    coords = [getattr(device, "coords", None) for device in row]
    if any(c is None for c in coords):
        return (count // 4, 2, 2) if count % 4 == 0 else (count, 1, 1)
    sizes = tuple(len({c[axis] for c in coords}) for axis in (2, 1, 0))
    if sizes[0] * sizes[1] * sizes[2] != count:
        return (count, 1, 1)
    return sizes


def gather_kernel(sizes, pieces, count, *refs):
    ins, outs = refs[:count], refs[count:-3]
    local_sem, send_sem, recv_sem = refs[-3:]
    me = lax.axis_index("sp")
    strides = (sizes[1] * sizes[2], sizes[2], 1)
    where = [lax.rem(me // strides[k], sizes[k]) for k in range(3)]
    wide = ins[0].shape[2] // HALVES

    def peer(axis, step):
        other = lax.rem(where[axis] + step, sizes[axis])
        return me + (other - where[axis]) * strides[axis]

    peers = [(axis, step) for axis in range(3) for step in range(1, sizes[axis])]
    barrier = pltpu.get_barrier_semaphore()
    for axis, step in peers:
        pl.semaphore_signal(barrier, inc=1, device_id={"sp": peer(axis, step)}, device_id_type=MESH)
    pl.semaphore_wait(barrier, len(peers))

    def source(piece):
        matrix, layer, half = pieces[piece][:3]
        return ins[matrix].at[layer, :, pl.ds(half * wide, wide)]

    def block(piece, done):
        half, phases, out, slot = pieces[piece][2:]
        order = ORDERS[half]
        if phases == 3:
            index = [slice(None) if axis in done else where[axis] for axis in range(3)]
            return outs[out].at[(*index, slice(None), pl.ds(half * wide, wide))]
        index = [slice(None) if axis in done else where[axis] for axis in order[:2]]
        return outs[out].at[(slot, *index, slice(None), slice(None))]

    def local(piece):
        return pltpu.make_async_copy(source(piece), block(piece, ()), local_sem.at[piece])

    def copies(piece, phase):
        order = ORDERS[pieces[piece][2]]
        if phase >= pieces[piece][3]:
            return []
        axis = order[phase]
        target = block(piece, order[:phase])
        found = []
        for step in range(1, sizes[axis]):
            slot = peers.index((axis, step))
            found.append(
                pltpu.make_async_remote_copy(
                    src_ref=source(piece) if phase == 0 else target,
                    dst_ref=target,
                    send_sem=send_sem.at[piece, slot],
                    recv_sem=recv_sem.at[piece, slot],
                    device_id={"sp": peer(axis, step)},
                    device_id_type=MESH,
                )
            )
        return found

    def start(piece, phase):
        if phase == 0:
            local(piece).start()
        for copy in copies(piece, phase):
            copy.start()

    def landed(piece, phase):
        if phase == 0:
            local(piece).wait()
        for copy in copies(piece, phase):
            copy.wait_recv()

    total = len(pieces)
    for piece in range(min(LOOKAHEAD, total)):
        start(piece, 0)
    for step in range(total + 1):
        if step + LOOKAHEAD < total:
            start(step + LOOKAHEAD, 0)
        if step < total:
            landed(step, 0)
            start(step, 1)
        if step >= 1:
            landed(step - 1, 1)
            start(step - 1, 2)
    for piece in range(total):
        landed(piece, 2)
        for phase in range(3):
            for copy in copies(piece, phase):
                copy.wait_send()


def gather_weights(sizes, weights, deferred):
    layers, depth, columns = weights[0].shape
    whole = layers - 1 if deferred else layers
    shapes, pieces = [], []
    for layer in range(whole):
        for matrix in range(3):
            for half in range(HALVES):
                pieces.append((matrix, layer, half, 3, len(shapes), 0))
            shapes.append((*sizes, depth, columns))
    if deferred:
        base = len(shapes)
        for group, members in enumerate(((0, 1), (2,))):
            for half in range(HALVES):
                ahead = tuple(sizes[axis] for axis in ORDERS[half][:2])
                shapes.append((len(members), *ahead, depth, columns // HALVES))
            for slot, matrix in enumerate(members):
                for half in range(HALVES):
                    out = base + group * HALVES + half
                    pieces.append((matrix, whole, half, 2, out, slot))
    slots = sum(size - 1 for size in sizes)
    gathered = pl.pallas_call(
        functools.partial(gather_kernel, sizes, pieces, len(weights)),
        out_shape=[jax.ShapeDtypeStruct(shape, jnp.bfloat16) for shape in shapes],
        in_specs=[pl.BlockSpec(memory_space=pltpu.VMEM)] * len(weights),
        out_specs=[pl.BlockSpec(memory_space=pl.ANY)] * len(shapes),
        scratch_shapes=[
            pltpu.SemaphoreType.DMA((len(pieces),)),
            pltpu.SemaphoreType.DMA((len(pieces), slots)),
            pltpu.SemaphoreType.DMA((len(pieces), slots)),
        ],
        compiler_params=pltpu.CompilerParams(collective_id=0, has_side_effects=True),
    )(*weights)
    rows = sizes[0] * sizes[1] * sizes[2] * depth
    full = [gathered[k].reshape(rows, columns) for k in range(3 * whole)]
    return full, gathered[3 * whole :]


def last_hop(stage, sizes, half):
    axis = ORDERS[half][2]
    stride = (sizes[1] * sizes[2], sizes[2], 1)[axis]
    count = sizes[0] * sizes[1] * sizes[2]
    pairs = [(i, i + stride if (i // stride) % 2 == 0 else i - stride) for i in range(count)]
    return lax.ppermute(stage, "sp", pairs)


def split_channels(block, sizes, half):
    axis = ORDERS[half][2]
    count = sizes[0] * sizes[1] * sizes[2]
    depth = block.shape[1] // count
    stride = (sizes[1] * sizes[2], sizes[2], 1)[axis]
    sides = [
        jnp.concatenate(
            [block[:, i * depth : (i + 1) * depth] for i in range(count) if (i // stride) % 2 == side],
            axis=1,
        )
        for side in range(2)
    ]
    first = lax.rem(lax.axis_index("sp") // stride, 2) == 0
    return jnp.where(first, sides[0], sides[1]), jnp.where(first, sides[1], sides[0])


def split_dot(parts, own, other):
    return jnp.dot(
        parts[0], own.reshape(-1, own.shape[-1]), preferred_element_type=jnp.float32
    ) + jnp.dot(parts[1], other.reshape(-1, other.shape[-1]), preferred_element_type=jnp.float32)


def with_halo(block, width):
    count = lax.axis_size("sp")
    forward = [(i, i + 1) for i in range(count - 1)]
    backward = [(target, source) for source, target in forward]
    low = lax.ppermute(block[block.shape[0] - width :], "sp", forward)
    high = lax.ppermute(block[:width], "sp", backward)
    return jnp.concatenate([low, block, high], axis=0)


def all_channels(block):
    if lax.axis_size("tp") != 2:
        return lax.all_gather(block, "tp", axis=1, tiled=True)
    other = lax.ppermute(block, "tp", [(0, 1), (1, 0)])
    first = lax.axis_index("tp") == 0
    return jnp.concatenate(
        [jnp.where(first, block, other), jnp.where(first, other, block)], axis=1
    )


def normalize_rows(stream_f, gain):
    factor = lax.rsqrt(jnp.mean(stream_f * stream_f, axis=1, keepdims=True) + EPSILON)
    return (stream_f * factor * gain[None, :]).astype(jnp.bfloat16)


def convolve(padded, kernel, conv_shift, out_rows):
    summed = jnp.zeros((out_rows, padded.shape[1]), jnp.float32) + conv_shift[None, :]
    for offset in range(kernel.shape[0]):
        window = lax.slice_in_dim(padded, offset, offset + out_rows, axis=0).astype(jnp.float32)
        summed = summed + window * kernel[offset][None, :]
    return summed


def finish_norm(conv_out, row_sum, row_squares, gain, shift):
    average = row_sum / D
    variance = row_squares / D - average * average
    normed = (conv_out - average) * lax.rsqrt(variance + EPSILON) * gain[None, :] + shift[None, :]
    return jax.nn.silu(normed).astype(jnp.bfloat16)


def local(
    sizes,
    stream,
    norm_gain,
    a_weight,
    gate_weight,
    conv_weight,
    conv_bias,
    ln_gain,
    ln_shift,
    out_weight,
):
    reach = (conv_weight.shape[1] - 1) // 2
    margin = (reach + ROUND - 1) // ROUND * ROUND
    layer_total = a_weight.shape[0]
    rows = stream.shape[0]
    deferred = sizes[1] == 2 and sizes[2] == 2 and layer_total > 1
    full, stages = gather_weights(sizes, (a_weight, gate_weight, out_weight), deferred)
    hops = []
    token = lax.axis_index("sp") * rows
    everything = rows * lax.axis_size("sp")
    spread = with_halo(all_channels(stream), margin * layer_total)
    wide = stream.shape[1]
    current = lax.dynamic_slice_in_dim(spread, lax.axis_index("tp") * wide, wide, axis=1)
    for layer_index in range(layer_total):
        beyond = margin * (layer_total - layer_index)
        if layer_index > 0:
            index = token - beyond + lax.broadcasted_iota(jnp.int32, (current.shape[0], 1), 0)
            inside = (index >= 0) & (index < everything)
            current = jnp.where(inside, current, jnp.zeros_like(current))
            spread = all_channels(current)
        stream_f = current.astype(jnp.float32)
        normed = normalize_rows(spread.astype(jnp.float32), norm_gain[layer_index])
        late = deferred and layer_index == layer_total - 1
        if late:
            gated = []
            for half in range(HALVES):
                parts = split_channels(normed, sizes, half)
                own, other = stages[half], hops[half]
                linear = split_dot(parts, own[0], other[0])
                gating = split_dot(parts, own[1], other[1])
                gated.append((linear * jax.nn.sigmoid(gating)).astype(jnp.bfloat16))
            gated = jnp.concatenate(gated, axis=1)
        else:
            matrices = full[3 * layer_index : 3 * layer_index + 3]
            linear = jnp.dot(normed, matrices[0], preferred_element_type=jnp.float32)
            gating = jnp.dot(normed, matrices[1], preferred_element_type=jnp.float32)
            gated = (linear * jax.nn.sigmoid(gating)).astype(jnp.bfloat16)
        if deferred and layer_index == layer_total - 2:
            hops = [last_hop(stages[half], sizes, half) for half in range(HALVES)]
            hops += [last_hop(stages[HALVES + half], sizes, half) for half in range(HALVES)]
        out_rows = rows + 2 * (beyond - margin)
        conv_out = convolve(
            gated[margin - reach :], conv_weight[layer_index], conv_bias[layer_index], out_rows
        )
        row_sum, row_squares = lax.psum(
            (
                jnp.sum(conv_out, axis=1, keepdims=True),
                jnp.sum(conv_out * conv_out, axis=1, keepdims=True),
            ),
            "tp",
        )
        mixed_in = finish_norm(
            conv_out, row_sum, row_squares, ln_gain[layer_index], ln_shift[layer_index]
        )
        mixed_rows = all_channels(mixed_in)
        if late:
            branch = jnp.concatenate(
                [
                    split_dot(
                        split_channels(mixed_rows, sizes, half),
                        stages[HALVES + half][0],
                        hops[HALVES + half][0],
                    )
                    for half in range(HALVES)
                ],
                axis=1,
            )
        else:
            branch = jnp.dot(mixed_rows, matrices[2], preferred_element_type=jnp.float32)
        kept = lax.slice_in_dim(stream_f, margin, margin + out_rows, axis=0)
        current = (kept + branch).astype(jnp.bfloat16)
    return current


def solution(mesh):
    placed = (
        P("sp", "tp"),
        P(),
        P(None, "sp", "tp"),
        P(None, "sp", "tp"),
        P(None, None, "tp"),
        P(None, "tp"),
        P(None, "tp"),
        P(None, "tp"),
        P(None, "sp", "tp"),
    )
    sizes = grid_of(mesh)

    def whole(*args):
        return local(sizes, *args)

    return jax.shard_map(
        whole, mesh=mesh, in_specs=placed, out_specs=P("sp", "tp"), check_vma=False
    )
```
